32 devices in a mesh: sp: 4 (over y, x), tp: 8 (over z, core).
Axes of the slice: x: 2, y: 2, z: 4, core: 2. Of those that a mesh axis runs over, the one named last changes fastest.
Arguments:
- stream: bfloat16 [2048, 1024], P('sp', 'tp'), may hold values from -6 to 6
- gain_first: bfloat16 [1024], P('tp'), may hold values from 0.099609375 to 1.8984375
- query_first: bfloat16 [1024, 1024], P('sp', 'tp'), may hold values from -0.1875 to 0.1875
- key_first: bfloat16 [1024, 1024], P('sp', 'tp'), may hold values from -0.1875 to 0.1875
- value_first: bfloat16 [1024, 1024], P('sp', 'tp'), may hold values from -0.1875 to 0.1875
- offset_first: float32 [8, 15, 31], P('tp'), may hold values from -4 to 254
- gain_second: bfloat16 [1024], P('tp'), may hold values from 0.099609375 to 1.8984375
- query_second: bfloat16 [1024, 1024], P('sp', 'tp'), may hold values from -0.1875 to 0.1875
- key_second: bfloat16 [1024, 1024], P('sp', 'tp'), may hold values from -0.1875 to 0.1875
- value_second: bfloat16 [1024, 1024], P('sp', 'tp'), may hold values from -0.1875 to 0.1875
- offset_second: float32 [8, 15, 31], P('tp'), may hold values from -4 to 254
Outputs:
- result: bfloat16 [2048, 1024], P('sp', 'tp')
The draws below stay inside these ranges and needn't reach their ends.
All inputs are finite; a program needn't handle non-finite values.
Results may differ from the reference program's by a relative error of at most 0.008.
Values may be sent and summed in bfloat16 or wider, within the bound.
A program may use at most 64 MiB of HBM per device.

```python
import jax
import jax.numpy as jnp
import numpy as np
from jax import lax

GRID_W = 64
HEAD_DIM = 128
HEADS = 8
D = 1024
TOKENS = 2048


def draw_stream(key, part):
    first, second = jax.random.split(jax.random.fold_in(key, 11))
    blocks = D // HEAD_DIM
    scales = jnp.exp(jax.random.uniform(first, (blocks,), jnp.float32, jnp.log(0.15), jnp.log(1.0)))
    base = jnp.clip(jax.random.normal(second, (TOKENS, D), jnp.float32), -6.0, 6.0)
    return (base * jnp.repeat(scales, HEAD_DIM)[None, :]).astype(jnp.bfloat16)


def draw_table(key):
    base = jnp.clip(jax.random.normal(key, (HEADS, 15, 31), jnp.float32), -4.0, 4.0)
    return base


def draw_offset_first(key, part):
    return draw_table(jax.random.fold_in(key, 21))


def draw_offset_second(key, part):
    return draw_table(jax.random.fold_in(key, 22))


def levels(key, dims, cuts, least, high):
    level = 1.0
    for axis_at, blocks in cuts:
        steps = jax.random.uniform(jax.random.fold_in(jax.random.fold_in(key, 6), axis_at), (blocks,), jnp.float32, least / len(cuts), high / len(cuts))
        level = level * jnp.repeat(jnp.exp(steps), dims[axis_at] // blocks).reshape((-1,) + (1,) * (len(dims) - 1 - axis_at))
    return level


def normal_values(key, shape, scale, bound, cuts=(), held_as=jnp.bfloat16):
    factor_of = levels(key, shape, cuts, -0.22, 0.18) if cuts else 1.0
    values = jax.random.normal(key, shape, jnp.float32) * scale * factor_of
    return jnp.minimum(jnp.maximum(values, -bound), bound).astype(held_as)


def setup_inputs(seed: int = 0) -> dict:
    key_of = jax.random.split(jax.random.key(seed), 12)
    stream = draw_stream(jax.random.fold_in(key_of[11], 71), 0)
    gain_first = jnp.clip(1.0 + 0.18 * jax.random.normal(key_of[1], (D,), jnp.float32), 0.099609375, 1.8984375).astype(jnp.bfloat16)
    query_first = normal_values(key_of[2], (D, D), D ** -0.5, 0.1875, ((0, 4), (1, 8)))
    key_first = normal_values(key_of[3], (D, D), D ** -0.5, 0.1875, ((0, 4), (1, 8)))
    value_first = normal_values(key_of[4], (D, D), D ** -0.5, 0.1875, ((0, 4), (1, 8)))
    offset_first = draw_offset_first(jax.random.fold_in(key_of[11], 71), 0)
    gain_second = jnp.clip(1.0 + 0.18 * jax.random.normal(key_of[6], (D,), jnp.float32), 0.099609375, 1.8984375).astype(jnp.bfloat16)
    query_second = normal_values(key_of[7], (D, D), D ** -0.5, 0.1875, ((0, 4), (1, 8)))
    key_second = normal_values(key_of[8], (D, D), D ** -0.5, 0.1875, ((0, 4), (1, 8)))
    value_second = normal_values(key_of[9], (D, D), D ** -0.5, 0.1875, ((0, 4), (1, 8)))
    offset_second = draw_offset_second(jax.random.fold_in(key_of[11], 71), 0)
    return {"stream": stream, "gain_first": gain_first, "query_first": query_first, "key_first": key_first, "value_first": value_first, "offset_first": offset_first, "gain_second": gain_second, "query_second": query_second, "key_second": key_second, "value_second": value_second, "offset_second": offset_second}


epsilon = 1e-06

def normalize(stream, gain):
    widened = stream.astype(jnp.float32)
    mean_square = lax.optimization_barrier(jnp.mean(widened * widened, axis=-1, keepdims=True))
    return (widened * lax.rsqrt(mean_square + epsilon) * gain.astype(jnp.float32)).astype(jnp.bfloat16)

def attend(query, keys, values, table, row_start, total_rows):
    rows_here, width, heads, head_size = query.shape
    blocks = width // 16
    query_cols = np.arange(width).reshape(blocks, 16)
    window_start = np.clip(query_cols - 8, 0, width - 16)
    key_cols = np.clip(np.arange(blocks) * 16 - 8, 0, width - 32)[:, None] + np.arange(32)
    column_ok = (key_cols[:, None, :] >= window_start[:, :, None]) & (key_cols[:, None, :] < window_start[:, :, None] + 16)
    column_offset = np.clip(key_cols[:, None, :] - query_cols[:, :, None] + 15, 0, 30)
    column_bias = table.astype(jnp.float32)[:, :, column_offset]
    mask = jnp.asarray(column_ok)[None, :, :, None, :]
    factor = head_size ** (-0.5)

    def one_row(index):
        grid_row = row_start + index
        first = jnp.clip(grid_row - 4, 0, total_rows - 8)
        local = first - row_start + 4
        key_block = lax.dynamic_slice_in_dim(keys, local, 8, 0)[:, key_cols].astype(jnp.float32)
        value_block = lax.dynamic_slice_in_dim(values, local, 8, 0)[:, key_cols].astype(jnp.float32)
        query_row = lax.dynamic_index_in_dim(query, index, 0, keepdims=False).reshape(blocks, 16, heads, head_size)
        scores = jnp.einsum('jqhe,mjkhe->hjqmk', query_row.astype(jnp.float32), key_block) * factor
        row_offset = first + jnp.arange(8, dtype=jnp.int32) - grid_row + 7
        row_bias = jnp.transpose(jnp.take(column_bias, row_offset, axis=1), (0, 2, 3, 1, 4))
        scores = jnp.where(mask, scores + row_bias, -1e+30)
        weight = jax.nn.softmax(scores.reshape(heads, blocks, 16, 256), axis=-1)
        rounded = weight.astype(jnp.bfloat16).reshape(heads, blocks, 16, 8, 32)
        output = jnp.einsum('hjqmk,mjkhe->jqhe', rounded.astype(jnp.float32), value_block)
        return output.reshape(width, heads * head_size)
    return lax.map(one_row, jnp.arange(rows_here, dtype=jnp.int32))

def layer(stream, gain, w_query, w_key, w_value, table):
    normed = normalize(stream, gain)
    query = jnp.dot(normed, w_query, preferred_element_type=jnp.float32).astype(jnp.bfloat16)
    keys = jnp.dot(normed, w_key, preferred_element_type=jnp.float32).astype(jnp.bfloat16)
    values = jnp.dot(normed, w_value, preferred_element_type=jnp.float32).astype(jnp.bfloat16)
    total_rows = stream.shape[0] // GRID_W
    shape = (total_rows, GRID_W, HEADS, HEAD_DIM)
    padding = ((4, 4), (0, 0), (0, 0), (0, 0))
    keys = jnp.pad(keys.reshape(shape), padding)
    values = jnp.pad(values.reshape(shape), padding)
    output = attend(query.reshape(shape), keys, values, table, 0, total_rows)
    return (stream.astype(jnp.float32) + output.reshape(stream.shape)).astype(jnp.bfloat16)

def reference(stream, gain_first, query_first, key_first, value_first, offset_first, gain_second, query_second, key_second, value_second, offset_second):
    middle = layer(stream, gain_first, query_first, key_first, value_first, offset_first)
    return layer(middle, gain_second, query_second, key_second, value_second, offset_second)
```

```python
import functools

import jax
import jax.numpy as jnp
from jax import lax
from jax.experimental import pallas as pl
from jax.experimental.pallas import tpu as pltpu
from jax.sharding import PartitionSpec as P

GRID_W = 64
WIN_R = 8
WIN_C = 16
HALO = 4
GAIN_ROWS = 16
epsilon = 1e-06
MESH = pl.DeviceIdType.MESH


def build_bias(table_ref, rows_ref, tiles_ref):
    rows_ref[...] = jnp.zeros_like(rows_ref)
    rows_ref[0 : 2 * WIN_R - 1, 0 : 2 * WIN_C - 1] = table_ref[0]
    shape = (GRID_W, 2 * GRID_W)
    column = lax.broadcasted_iota(jnp.int32, shape, 0)
    key_column = lax.broadcasted_iota(jnp.int32, shape, 1)
    key_column = jnp.where(key_column >= GRID_W, key_column - GRID_W, key_column)
    start = jnp.clip(column - WIN_C // 2, 0, GRID_W - WIN_C)
    inside = (key_column >= start) & (key_column < start + WIN_C)
    for o in range(2 * WIN_R - 2):
        pair = rows_ref[o : o + 1, :] + pltpu.roll(rows_ref[o + 1 : o + 2, :], GRID_W, 1)
        tile = pltpu.roll(
            jnp.broadcast_to(pair, shape), 2 * GRID_W - (WIN_C - 1), 1, stride=1, stride_axis=0
        )
        tiles_ref[o] = jnp.where(inside, tile, -1e30)


def kernel(
    n_sp,
    n_tp,
    x_ref,
    gains_ref,
    wq_a,
    wk_a,
    wv_a,
    wq_b,
    wk_b,
    wv_b,
    table_a,
    table_b,
    out_ref,
    xg_a,
    xg_b,
    wkv_a,
    wkv_b,
    wqg_a,
    wqg_b,
    kvp_a,
    kvp_b,
    q_buf,
    normed,
    rows_buf,
    tiles_a,
    tiles_b,
    load_sem,
    xs_sem,
    xr_sem,
    ws_sem,
    wr_sem,
    hs_sem,
    hr_sem,
):
    sp = lax.axis_index("sp")
    tp = lax.axis_index("tp")
    tokens, feat = x_ref.shape
    depth = wq_a.shape[0]
    rows_dev = tokens // GRID_W
    total_rows = rows_dev * n_sp
    half = n_tp // 2
    core = lax.rem(tp, 2)
    partner = tp + 1 - 2 * core
    low = HALO * GRID_W
    below = (HALO - 1 if rows_dev >= WIN_R else HALO) * GRID_W
    factor = feat ** (-0.5)

    xg = (xg_a, xg_b)
    wkv = (wkv_a, wkv_b)
    wqg = (wqg_a, wqg_b)
    kvp = (kvp_a, kvp_b)
    tiles = (tiles_a, tiles_b)

    def w_rows(device):
        return pl.ds(pl.multiple_of(device * depth, depth), depth)

    mine = w_rows(sp)
    loads = [
        (x_ref, xg_a.at[tp, pl.ds(0, tokens)]),
        (gains_ref, xg_a.at[tp, pl.ds(tokens, GAIN_ROWS)]),
        (wk_a, wkv_a.at[mine, pl.ds(0, feat)]),
        (wv_a, wkv_a.at[mine, pl.ds(feat, feat)]),
        (wq_a, wqg_a.at[mine]),
        (wk_b, wkv_b.at[mine, pl.ds(0, feat)]),
        (wv_b, wkv_b.at[mine, pl.ds(feat, feat)]),
        (wq_b, wqg_b.at[mine]),
    ]
    loads = [pltpu.make_async_copy(s, d, load_sem.at[i]) for i, (s, d) in enumerate(loads)]
    for load in loads:
        load.start()

    barrier = pltpu.get_barrier_semaphore()
    chip_peers = [lax.rem(tp + 2 * k, n_tp) for k in range(1, half)]
    chip_sources = [lax.rem(tp + n_tp - 2 * k, n_tp) for k in range(1, half)]
    sp_peers = [lax.rem(sp + k, n_sp) for k in range(1, n_sp)]
    sp_sources = [lax.rem(sp + n_sp - k, n_sp) for k in range(1, n_sp)]
    for t in [partner] + chip_peers:
        pl.semaphore_signal(barrier, inc=1, device_id=(sp, t), device_id_type=MESH)
    for s in sp_peers:
        pl.semaphore_signal(barrier, inc=1, device_id=(s, tp), device_id_type=MESH)
    pl.semaphore_wait(barrier, half + n_sp - 1)

    def remote(src, dst, send, recv, device):
        return pltpu.make_async_remote_copy(
            src_ref=src,
            dst_ref=dst,
            send_sem=send,
            recv_sem=recv,
            device_id=device,
            device_id_type=MESH,
        )

    sent = []

    def x_slot(layer, slot):
        if layer == 0:
            return xg[0].at[slot]
        return xg[1].at[slot]

    def x_copy(layer, slot, index, target):
        ref = x_slot(layer, slot)
        return remote(ref, ref, xs_sem.at[layer, index], xr_sem.at[layer, slot], (sp, target))

    def x_start(layer):
        for index, target in enumerate(chip_peers + [partner]):
            copy = x_copy(layer, tp, index, target)
            copy.start()
            sent.append(copy)

    def x_finish(layer):
        for index, slot in enumerate(chip_sources):
            x_copy(layer, slot, half + index, partner).wait_recv()
            copy = x_copy(layer, slot, half + index, partner)
            copy.start()
            sent.append(copy)
        for k in range(half):
            slot = lax.rem(partner + n_tp - 2 * k, n_tp)
            x_copy(layer, slot, 0, partner).wait_recv()

    def w_copy(layer, which, slot, index, target):
        ref = (wkv, wqg)[which][layer].at[w_rows(slot)]
        return remote(
            ref, ref, ws_sem.at[layer, which, index], wr_sem.at[layer, which, slot], (target, tp)
        )

    def w_start(layer, which):
        for index, target in enumerate(sp_peers):
            copy = w_copy(layer, which, sp, index, target)
            copy.start()
            sent.append(copy)

    def w_finish(layer, which):
        for slot in sp_sources:
            w_copy(layer, which, slot, 0, slot).wait_recv()

    def down(layer):
        buf = kvp[layer]
        return remote(
            buf.at[pl.ds(tokens, low)],
            buf.at[pl.ds(0, low)],
            hs_sem.at[layer, 0],
            hr_sem.at[layer, 0],
            (lax.rem(sp + 1, n_sp), tp),
        )

    def up(layer):
        buf = kvp[layer]
        return remote(
            buf.at[pl.ds(low, below)],
            buf.at[pl.ds(low + tokens, below)],
            hs_sem.at[layer, 1],
            hr_sem.at[layer, 1],
            (lax.rem(sp + n_sp - 1, n_sp), tp),
        )

    has_next = sp < n_sp - 1
    has_previous = sp > 0

    def norm(layer):
        chunk = GRID_W
        buf = xg[layer]
        for c in range(tokens // chunk):
            at = pl.ds(c * chunk, chunk)
            total = jnp.zeros((chunk, feat), jnp.float32)
            for s in range(n_tp):
                wide = buf[s, at, :].astype(jnp.float32)
                total = total + wide * wide
            mean = jnp.sum(total, axis=-1, keepdims=True) * (1.0 / (n_tp * feat))
            scale = lax.rsqrt(mean + epsilon)
            for s in range(n_tp):
                gain = xg_a[s, pl.ds(tokens, GAIN_ROWS), :][layer : layer + 1, :]
                wide = buf[s, at, :].astype(jnp.float32)
                normed[at, s * feat : (s + 1) * feat] = (
                    wide * scale * gain.astype(jnp.float32)
                ).astype(jnp.bfloat16)

    def project(weights, dst, offset):
        chunk = 2 * GRID_W if tokens % (2 * GRID_W) == 0 else GRID_W
        for c in range(tokens // chunk):
            made = jnp.dot(
                normed[c * chunk : (c + 1) * chunk, :],
                weights[...],
                preferred_element_type=jnp.float32,
            )
            dst[pl.ds(offset + c * chunk, chunk), :] = made.astype(jnp.bfloat16)

    def attend(layer, index):
        row = sp * rows_dev + index
        first = jnp.minimum(jnp.maximum(row - HALO, 0), total_rows - WIN_R)
        local = first - sp * rows_dev + HALO
        base = first - row + WIN_R - 1
        at = pl.ds(pl.multiple_of(local * GRID_W, GRID_W), WIN_R * GRID_W)
        keys = kvp[layer][at, 0:feat]
        values = kvp[layer][at, feat : 2 * feat]
        query = q_buf[index * GRID_W : (index + 1) * GRID_W, :]
        scores = lax.dot_general(
            query, keys, (((1,), (1,)), ((), ())), preferred_element_type=jnp.float32
        )
        bias = jnp.concatenate([tiles[layer][base + 2 * j] for j in range(WIN_R // 2)], axis=1)
        scores = scores * factor + bias
        top = jnp.max(scores, axis=-1, keepdims=True)
        weight = jnp.exp(scores - top)
        weight = weight * (1.0 / jnp.sum(weight, axis=-1, keepdims=True))
        out = jnp.dot(weight.astype(jnp.bfloat16), values, preferred_element_type=jnp.float32)
        here = pl.ds(index * GRID_W, GRID_W)
        wide = xg[layer][tp, here, :].astype(jnp.float32)
        return (wide + out).astype(jnp.bfloat16)

    loads[0].wait()
    loads[1].wait()
    x_start(0)
    loads[2].wait()
    loads[3].wait()
    w_start(0, 0)
    loads[4].wait()
    w_start(0, 1)
    build_bias(table_a, rows_buf, tiles_a)
    build_bias(table_b, rows_buf, tiles_b)
    for load in loads[5:]:
        load.wait()

    for layer in range(2):
        x_finish(layer)
        norm(layer)
        w_finish(layer, 0)
        project(wkv[layer], kvp[layer], low)

        @pl.when(has_next)
        def _():
            down(layer).start()

        @pl.when(has_previous)
        def _():
            up(layer).start()

        if layer == 0:
            w_start(1, 0)
            w_start(1, 1)
        w_finish(layer, 1)
        project(wqg[layer], q_buf, 0)

        @pl.when(has_previous)
        def _():
            down(layer).wait_recv()

        @pl.when(has_next)
        def _():
            up(layer).wait_recv()

        for index in range(rows_dev):
            made = attend(layer, index)
            here = pl.ds(index * GRID_W, GRID_W)
            if layer == 0:
                xg_b[tp, here, :] = made
            else:
                out_ref[here, :] = made
        if layer == 0:
            x_start(1)

    for layer in range(2):

        @pl.when(has_next)
        def _():
            down(layer).wait_send()

        @pl.when(has_previous)
        def _():
            up(layer).wait_send()

    for copy in sent:
        copy.wait_send()


def body(n_sp, n_tp, stream, gain_a, wq_a, wk_a, wv_a, table_a, gain_b, wq_b, wk_b, wv_b, table_b):
    tokens, feat = stream.shape
    depth = wq_a.shape[0] * n_sp
    gains = jnp.pad(jnp.stack([gain_a, gain_b]), ((0, GAIN_ROWS - 2), (0, 0)))
    bf16 = jnp.bfloat16
    padded = tokens + 2 * HALO * GRID_W
    hbm = pl.BlockSpec(memory_space=pl.ANY)
    vmem = pl.BlockSpec(memory_space=pltpu.VMEM)
    dma = pltpu.SemaphoreType.DMA
    return pl.pallas_call(
        functools.partial(kernel, n_sp, n_tp),
        out_shape=jax.ShapeDtypeStruct((tokens, feat), bf16),
        in_specs=[hbm] * 8 + [vmem] * 2,
        out_specs=vmem,
        scratch_shapes=[
            pltpu.VMEM((n_tp, tokens + GAIN_ROWS, feat), bf16),
            pltpu.VMEM((n_tp, tokens, feat), bf16),
            pltpu.VMEM((depth, 2 * feat), bf16),
            pltpu.VMEM((depth, 2 * feat), bf16),
            pltpu.VMEM((depth, feat), bf16),
            pltpu.VMEM((depth, feat), bf16),
            pltpu.VMEM((padded, 2 * feat), bf16),
            pltpu.VMEM((padded, 2 * feat), bf16),
            pltpu.VMEM((tokens, feat), bf16),
            pltpu.VMEM((tokens, n_tp * feat), bf16),
            pltpu.VMEM((2 * WIN_R, 2 * GRID_W), jnp.float32),
            pltpu.VMEM((2 * WIN_R - 2, GRID_W, 2 * GRID_W), jnp.float32),
            pltpu.VMEM((2 * WIN_R - 2, GRID_W, 2 * GRID_W), jnp.float32),
            dma((8,)),
            dma((2, n_tp)),
            dma((2, n_tp)),
            dma((2, 2, n_sp)),
            dma((2, 2, n_sp)),
            dma((2, 2)),
            dma((2, 2)),
        ],
        compiler_params=pltpu.CompilerParams(collective_id=0, has_side_effects=True),
    )(stream, gains, wq_a, wk_a, wv_a, wq_b, wk_b, wv_b, table_a, table_b)


def solution(mesh):
    placed = (
        P("sp", "tp"),
        P("tp"),
        P("sp", "tp"),
        P("sp", "tp"),
        P("sp", "tp"),
        P("tp", None, None),
        P("tp"),
        P("sp", "tp"),
        P("sp", "tp"),
        P("sp", "tp"),
        P("tp", None, None),
    )
    return jax.shard_map(
        functools.partial(body, mesh.shape["sp"], mesh.shape["tp"]),
        mesh=mesh,
        in_specs=placed,
        out_specs=P("sp", "tp"),
        check_vma=False,
    )
```

```python
import functools

import jax
import jax.numpy as jnp
from jax import lax
from jax.experimental import pallas as pl
from jax.experimental.pallas import tpu as pltpu
from jax.sharding import PartitionSpec as P

GRID_W = 64
WIN_R = 8
WIN_C = 16
HALO = 4
GAIN_ROWS = 16
epsilon = 1e-06
MESH = pl.DeviceIdType.MESH


def build_bias(table_ref, rows_ref, tiles_ref):
    rows_ref[...] = jnp.zeros_like(rows_ref)
    rows_ref[0 : 2 * WIN_R - 1, 0 : 2 * WIN_C - 1] = table_ref[:, 0, :]
    shape = (GRID_W, 2 * GRID_W)
    column = lax.broadcasted_iota(jnp.int32, shape, 0)
    key_column = lax.broadcasted_iota(jnp.int32, shape, 1)
    key_column = jnp.where(key_column >= GRID_W, key_column - GRID_W, key_column)
    start = jnp.clip(column - WIN_C // 2, 0, GRID_W - WIN_C)
    inside = (key_column >= start) & (key_column < start + WIN_C)
    for o in range(2 * WIN_R - 2):
        pair = rows_ref[o : o + 1, :] + pltpu.roll(rows_ref[o + 1 : o + 2, :], GRID_W, 1)
        tile = pltpu.roll(
            jnp.broadcast_to(pair, shape), 2 * GRID_W - (WIN_C - 1), 1, stride=1, stride_axis=0
        )
        tiles_ref[o] = jnp.where(inside, tile, -1e30)


def kernel(
    n_sp,
    n_tp,
    x_ref,
    gain_a,
    gain_b,
    wq_a,
    wk_a,
    wv_a,
    wq_b,
    wk_b,
    wv_b,
    table_a,
    table_b,
    out_ref,
    xg_a,
    xg_b,
    wkv_a,
    wkv_b,
    wqg_a,
    wqg_b,
    kvp_a,
    kvp_b,
    q_buf,
    normed,
    rows_buf,
    tiles_a,
    tiles_b,
    load_sem,
    xs_sem,
    xf_sem,
    xl_sem,
    xr_sem,
    ws_sem,
    wr_sem,
    hs_sem,
    hr_sem,
):
    sp = lax.axis_index("sp")
    tp = lax.axis_index("tp")
    tokens, feat = x_ref.shape
    depth = wq_a.shape[0]
    rows_dev = tokens // GRID_W
    total_rows = rows_dev * n_sp
    half = n_tp // 2
    core = lax.rem(tp, 2)
    z = tp // 2
    group = 2 if rows_dev % 2 == 0 else 1
    chunk = group * GRID_W
    count = rows_dev // group
    low_half = tuple(range(count // 2, count)) + tuple(range(count // 2))
    orders = (low_half, tuple(range(count)))
    partner = tp + 1 - 2 * core
    low = HALO * GRID_W
    below = (HALO - 1 if rows_dev >= WIN_R else HALO) * GRID_W
    factor = feat ** (-0.5)

    xg = (xg_a, xg_b)
    wkv = (wkv_a, wkv_b)
    wqg = (wqg_a, wqg_b)
    kvp = (kvp_a, kvp_b)
    tiles = (tiles_a, tiles_b)

    def w_rows(device):
        return pl.ds(pl.multiple_of(device * depth, depth), depth)

    mine = w_rows(sp)
    def place(layer, part):
        if layer == 1:
            return part * chunk
        return GAIN_ROWS + orders[0].index(part) * chunk

    loads = [
        (x_ref.at[pl.ds(part * chunk, chunk)], xg_a.at[tp, pl.ds(place(0, part), chunk)])
        for part in orders[0]
    ] + [
        (wk_a, wkv_a.at[mine, pl.ds(0, feat)]),
        (wv_a, wkv_a.at[mine, pl.ds(feat, feat)]),
        (wq_a, wqg_a.at[mine]),
        (wk_b, wkv_b.at[mine, pl.ds(0, feat)]),
        (wv_b, wkv_b.at[mine, pl.ds(feat, feat)]),
        (wq_b, wqg_b.at[mine]),
    ]
    loads = [pltpu.make_async_copy(s, d, load_sem.at[i]) for i, (s, d) in enumerate(loads)]
    for load in loads:
        load.start()
    spare = jnp.zeros((GAIN_ROWS - 2, feat), jnp.float32)
    both = [gain_a[...].astype(jnp.float32), gain_b[...].astype(jnp.float32), spare]
    xg_a[tp, 0:GAIN_ROWS, :] = jnp.concatenate(both, axis=0).astype(jnp.bfloat16)

    barrier = pltpu.get_barrier_semaphore()
    chip_peers = [lax.rem(tp + 2 * k, n_tp) for k in range(1, half)]
    sp_peers = [lax.rem(sp + k, n_sp) for k in range(1, n_sp)]
    sp_sources = [lax.rem(sp + n_sp - k, n_sp) for k in range(1, n_sp)]
    for t in [partner] + chip_peers:
        pl.semaphore_signal(barrier, inc=1, device_id=(sp, t), device_id_type=MESH)
    for s in sp_peers:
        pl.semaphore_signal(barrier, inc=1, device_id=(s, tp), device_id_type=MESH)
    pl.semaphore_wait(barrier, half + n_sp - 1)

    def remote(src, dst, send, recv, device):
        return pltpu.make_async_remote_copy(
            src_ref=src,
            dst_ref=dst,
            send_sem=send,
            recv_sem=recv,
            device_id=device,
            device_id_type=MESH,
        )

    sent = []

    def x_copy(layer, part, slot, sem, target):
        at, size = place(layer, part), chunk
        if layer == 0 and part == orders[0][0]:
            at, size = 0, chunk + GAIN_ROWS
        ref = xg[layer].at[slot, pl.ds(at, size)]
        return remote(ref, ref, sem, xr_sem.at[layer, part, slot], (sp, target))

    def begin(copy, condition=None):
        sent.append((copy, condition))
        if condition is None:
            copy.start()
        else:
            pl.when(condition)(copy.start)

    def x_start(layer, part):
        begin(x_copy(layer, part, tp, xf_sem.at[layer, part, tp], partner))
        for k in range(half - 1, 0, -1):
            right = z + k <= half - 2
            left = z - k >= 1
            if k == 1:
                right = right | (z == half - 2)
                left = left | (z == 1)
            sem = xs_sem.at[layer, part, k]
            begin(x_copy(layer, part, tp, sem, tp + 2 * k), right)
            sem = xs_sem.at[layer, part, half + k]
            begin(x_copy(layer, part, tp, sem, tp - 2 * k), left)

    def x_finish(layer, part):
        for k in range(1, half):
            slot = lax.rem(tp + 2 * k, n_tp)
            relay = xl_sem.at[layer, part, slot]
            x_copy(layer, part, slot, relay, partner).wait_recv()
            right = x_copy(layer, part, slot, relay, tp + 2)
            begin(right, (slot < tp) & (z == half - 2))
            left = x_copy(layer, part, slot, relay, tp - 2)
            begin(left, (slot > tp) & (z == 1))
            begin(x_copy(layer, part, slot, xf_sem.at[layer, part, slot], partner))
        for k in range(half):
            slot = lax.rem(partner + 2 * k, n_tp)
            x_copy(layer, part, slot, xf_sem.at[layer, part, slot], partner).wait_recv()

    def w_copy(layer, which, slot, index, target):
        ref = (wkv, wqg)[which][layer].at[w_rows(slot)]
        return remote(
            ref, ref, ws_sem.at[layer, which, index], wr_sem.at[layer, which, slot], (target, tp)
        )

    def w_start(layer, which):
        for index, target in enumerate(sp_peers):
            begin(w_copy(layer, which, sp, index, target))

    def w_finish(layer, which):
        for slot in sp_sources:
            w_copy(layer, which, slot, 0, slot).wait_recv()

    def down(layer):
        buf = kvp[layer]
        return remote(
            buf.at[pl.ds(tokens, low)],
            buf.at[pl.ds(0, low)],
            hs_sem.at[layer, 0],
            hr_sem.at[layer, 0],
            (lax.rem(sp + 1, n_sp), tp),
        )

    def up(layer):
        buf = kvp[layer]
        return remote(
            buf.at[pl.ds(low, below)],
            buf.at[pl.ds(low + tokens, below)],
            hs_sem.at[layer, 1],
            hr_sem.at[layer, 1],
            (lax.rem(sp + n_sp - 1, n_sp), tp),
        )

    has_next = sp < n_sp - 1
    has_previous = sp > 0

    def norm(layer, part):
        buf = xg[layer]
        for c in range(group):
            at = pl.ds(place(layer, part) + c * GRID_W, GRID_W)
            to = pl.ds(part * chunk + c * GRID_W, GRID_W)
            total = jnp.zeros((GRID_W, feat), jnp.float32)
            for s in range(n_tp):
                wide = buf[s, at, :].astype(jnp.float32)
                total = total + wide * wide
            mean = jnp.sum(total, axis=-1, keepdims=True) * (1.0 / (n_tp * feat))
            scale = lax.rsqrt(mean + epsilon)
            for s in range(n_tp):
                gain = xg_a[s, 0:GAIN_ROWS, :][layer : layer + 1, :]
                wide = buf[s, at, :].astype(jnp.float32)
                normed[to, s * feat : (s + 1) * feat] = (
                    wide * scale * gain.astype(jnp.float32)
                ).astype(jnp.bfloat16)

    def project(weights, dst, offset, part):
        made = jnp.dot(
            normed[part * chunk : (part + 1) * chunk, :],
            weights[...],
            preferred_element_type=jnp.float32,
        )
        dst[pl.ds(offset + part * chunk, chunk), :] = made.astype(jnp.bfloat16)

    def attend(layer, index):
        row = sp * rows_dev + index
        first = jnp.minimum(jnp.maximum(row - HALO, 0), total_rows - WIN_R)
        local = first - sp * rows_dev + HALO
        base = first - row + WIN_R - 1
        at = pl.ds(pl.multiple_of(local * GRID_W, GRID_W), WIN_R * GRID_W)
        keys = kvp[layer][at, 0:feat]
        values = kvp[layer][at, feat : 2 * feat]
        query = q_buf[index * GRID_W : (index + 1) * GRID_W, :]
        scores = lax.dot_general(
            query, keys, (((1,), (1,)), ((), ())), preferred_element_type=jnp.float32
        )
        bias = jnp.concatenate([tiles[layer][base + 2 * j] for j in range(WIN_R // 2)], axis=1)
        scores = scores * factor + bias
        top = jnp.max(scores, axis=-1, keepdims=True)
        weight = jnp.exp(scores - top)
        weight = weight * (1.0 / jnp.sum(weight, axis=-1, keepdims=True))
        out = jnp.dot(weight.astype(jnp.bfloat16), values, preferred_element_type=jnp.float32)
        start = place(layer, index // group) + index % group * GRID_W
        wide = xg[layer][tp, pl.ds(start, GRID_W), :].astype(jnp.float32)
        return (wide + out).astype(jnp.bfloat16)

    for load, part in zip(loads, orders[0]):
        load.wait()
        x_start(0, part)
    rest = loads[count:]
    rest[0].wait()
    rest[1].wait()
    w_start(0, 0)
    rest[2].wait()
    w_start(0, 1)
    build_bias(table_a, rows_buf, tiles_a)
    build_bias(table_b, rows_buf, tiles_b)
    for load in rest[3:]:
        load.wait()

    top_rows = [i for i in range(rows_dev) if i < HALO]
    end_rows = [i for i in range(rows_dev) if i + HALO > rows_dev]
    up_parts = {i // group for i in range(below // GRID_W)}
    down_parts = {i // group for i in range(rows_dev - HALO, rows_dev)}

    for layer in range(2):
        done = set()
        for part in orders[layer]:
            x_finish(layer, part)
            norm(layer, part)
            if not done:
                w_finish(layer, 0)
            project(wkv[layer], kvp[layer], low, part)
            before = set(done)
            done.add(part)
            if down_parts <= done and not down_parts <= before:
                pl.when(has_next)(down(layer).start)
            if up_parts <= done and not up_parts <= before:
                pl.when(has_previous)(up(layer).start)
        if layer == 0:
            w_start(1, 0)
            w_start(1, 1)
        w_finish(layer, 1)
        for part in orders[layer]:
            project(wqg[layer], q_buf, 0, part)

        late = end_rows if layer == 0 else top_rows
        early = top_rows if layer == 0 else end_rows
        early = [i for i in early if i not in late]
        inner = [i for i in range(rows_dev) if i not in late and i not in early]
        finished = set()
        for rows, wait in ((inner, None), (early, layer == 0), (late, layer == 1)):
            if wait is True:
                pl.when(has_previous)(down(layer).wait_recv)
            if wait is False:
                pl.when(has_next)(up(layer).wait_recv)
            for index in rows:
                made = attend(layer, index)
                here = pl.ds(index * GRID_W, GRID_W)
                if layer == 1:
                    out_ref[here, :] = made
                    continue
                xg_b[tp, here, :] = made
                finished.add(index)
                part = index // group
                if all(part * group + i in finished for i in range(group)):
                    x_start(1, part)

    for layer in range(2):
        pl.when(has_next)(down(layer).wait_send)
        pl.when(has_previous)(up(layer).wait_send)
    for copy, condition in sent:
        if condition is None:
            copy.wait_send()
        else:
            pl.when(condition)(copy.wait_send)


def body(n_sp, n_tp, stream, gain_a, wq_a, wk_a, wv_a, table_a, gain_b, wq_b, wk_b, wv_b, table_b):
    tokens, feat = stream.shape
    depth = wq_a.shape[0] * n_sp
    rows_dev = tokens // GRID_W
    parts = rows_dev // 2 if rows_dev % 2 == 0 else rows_dev
    bf16 = jnp.bfloat16
    padded = tokens + 2 * HALO * GRID_W
    hbm = pl.BlockSpec(memory_space=pl.ANY)
    vmem = pl.BlockSpec(memory_space=pltpu.VMEM)
    dma = pltpu.SemaphoreType.DMA
    return pl.pallas_call(
        functools.partial(kernel, n_sp, n_tp),
        out_shape=jax.ShapeDtypeStruct((tokens, feat), bf16),
        in_specs=[hbm] + [vmem] * 2 + [hbm] * 6 + [vmem] * 2,
        out_specs=vmem,
        scratch_shapes=[
            pltpu.VMEM((n_tp, tokens + GAIN_ROWS, feat), bf16),
            pltpu.VMEM((n_tp, tokens, feat), bf16),
            pltpu.VMEM((depth, 2 * feat), bf16),
            pltpu.VMEM((depth, 2 * feat), bf16),
            pltpu.VMEM((depth, feat), bf16),
            pltpu.VMEM((depth, feat), bf16),
            pltpu.VMEM((padded, 2 * feat), bf16),
            pltpu.VMEM((padded, 2 * feat), bf16),
            pltpu.VMEM((tokens, feat), bf16),
            pltpu.VMEM((tokens, n_tp * feat), bf16),
            pltpu.VMEM((2 * WIN_R, 2 * GRID_W), jnp.float32),
            pltpu.VMEM((2 * WIN_R - 2, GRID_W, 2 * GRID_W), jnp.float32),
            pltpu.VMEM((2 * WIN_R - 2, GRID_W, 2 * GRID_W), jnp.float32),
            dma((parts + 6,)),
            dma((2, parts, n_tp)),
            dma((2, parts, n_tp)),
            dma((2, parts, n_tp)),
            dma((2, parts, n_tp)),
            dma((2, 2, n_sp)),
            dma((2, 2, n_sp)),
            dma((2, 2)),
            dma((2, 2)),
        ],
        compiler_params=pltpu.CompilerParams(collective_id=0, has_side_effects=True),
    )(
        stream,
        gain_a.reshape(1, feat),
        gain_b.reshape(1, feat),
        wq_a,
        wk_a,
        wv_a,
        wq_b,
        wk_b,
        wv_b,
        jnp.transpose(table_a, (1, 0, 2)),
        jnp.transpose(table_b, (1, 0, 2)),
    )


def solution(mesh):
    placed = (
        P("sp", "tp"),
        P("tp"),
        P("sp", "tp"),
        P("sp", "tp"),
        P("sp", "tp"),
        P("tp", None, None),
        P("tp"),
        P("sp", "tp"),
        P("sp", "tp"),
        P("sp", "tp"),
        P("tp", None, None),
    )
    return jax.shard_map(
        functools.partial(body, mesh.shape["sp"], mesh.shape["tp"]),
        mesh=mesh,
        in_specs=placed,
        out_specs=P("sp", "tp"),
        check_vma=False,
    )
```

```python
import functools

import jax
import jax.numpy as jnp
from jax import lax
from jax.experimental import pallas as pl
from jax.experimental.pallas import tpu as pltpu
from jax.sharding import PartitionSpec as P

GRID_W = 64
WIN_R = 8
WIN_C = 16
HALO = 4
GAIN_ROWS = 16
epsilon = 1e-06
MESH = pl.DeviceIdType.MESH


def build_bias(table_ref, rows_ref, tiles_ref):
    rows_ref[...] = jnp.zeros_like(rows_ref)
    rows_ref[0 : 2 * WIN_R - 1, 0 : 2 * WIN_C - 1] = table_ref[:, 0, :]
    shape = (GRID_W, 2 * GRID_W)
    column = lax.broadcasted_iota(jnp.int32, shape, 0)
    key_column = lax.broadcasted_iota(jnp.int32, shape, 1)
    key_column = jnp.where(key_column >= GRID_W, key_column - GRID_W, key_column)
    start = jnp.clip(column - WIN_C // 2, 0, GRID_W - WIN_C)
    inside = (key_column >= start) & (key_column < start + WIN_C)
    for o in range(2 * WIN_R - 2):
        pair = rows_ref[o : o + 1, :] + pltpu.roll(rows_ref[o + 1 : o + 2, :], GRID_W, 1)
        tile = pltpu.roll(
            jnp.broadcast_to(pair, shape), 2 * GRID_W - (WIN_C - 1), 1, stride=1, stride_axis=0
        )
        tiles_ref[o] = jnp.where(inside, tile, -1e30)


def kernel(
    n_sp,
    n_tp,
    x_ref,
    gain_a,
    gain_b,
    wq_a,
    wk_a,
    wv_a,
    wq_b,
    wk_b,
    wv_b,
    table_a,
    table_b,
    out_ref,
    xg_a,
    xg_b,
    wkv_a,
    wkv_b,
    wqg_a,
    wqg_b,
    kvp_a,
    kvp_b,
    q_buf,
    normed,
    rows_buf,
    tiles_a,
    tiles_b,
    load_sem,
    xs_sem,
    xf_sem,
    xl_sem,
    xr_sem,
    ws_sem,
    wr_sem,
    hs_sem,
    hr_sem,
):
    sp = lax.axis_index("sp")
    tp = lax.axis_index("tp")
    tokens, feat = x_ref.shape
    depth = wq_a.shape[0]
    rows_dev = tokens // GRID_W
    total_rows = rows_dev * n_sp
    half = n_tp // 2
    core = lax.rem(tp, 2)
    z = tp // 2
    group = rows_dev // 2 if rows_dev % 2 == 0 else 1
    chunk = group * GRID_W
    count = rows_dev // group
    low_half = tuple(range(count // 2, count)) + tuple(range(count // 2))
    orders = (low_half, tuple(range(count)))
    partner = tp + 1 - 2 * core
    low = HALO * GRID_W
    below = (HALO - 1 if rows_dev >= WIN_R else HALO) * GRID_W
    factor = feat ** (-0.5)

    xg = (xg_a, xg_b)
    wkv = (wkv_a, wkv_b)
    wqg = (wqg_a, wqg_b)
    kvp = (kvp_a, kvp_b)
    tiles = (tiles_a, tiles_b)

    def w_rows(device):
        return pl.ds(pl.multiple_of(device * depth, depth), depth)

    mine = w_rows(sp)
    def place(layer, part):
        if layer == 1:
            return part * chunk
        return GAIN_ROWS + orders[0].index(part) * chunk

    loads = [
        (x_ref.at[pl.ds(part * chunk, chunk)], xg_a.at[tp, pl.ds(place(0, part), chunk)])
        for part in orders[0]
    ] + [
        (wk_a, wkv_a.at[mine, pl.ds(0, feat)]),
        (wv_a, wkv_a.at[mine, pl.ds(feat, feat)]),
        (wq_a, wqg_a.at[mine]),
        (wk_b, wkv_b.at[mine, pl.ds(0, feat)]),
        (wv_b, wkv_b.at[mine, pl.ds(feat, feat)]),
        (wq_b, wqg_b.at[mine]),
    ]
    loads = [pltpu.make_async_copy(s, d, load_sem.at[i]) for i, (s, d) in enumerate(loads)]
    for load in loads:
        load.start()
    spare = jnp.zeros((GAIN_ROWS - 2, feat), jnp.float32)
    both = [gain_a[...].astype(jnp.float32), gain_b[...].astype(jnp.float32), spare]
    xg_a[tp, 0:GAIN_ROWS, :] = jnp.concatenate(both, axis=0).astype(jnp.bfloat16)

    barrier = pltpu.get_barrier_semaphore()
    chip_peers = [lax.rem(tp + 2 * k, n_tp) for k in range(1, half)]
    sp_peers = [lax.rem(sp + k, n_sp) for k in range(1, n_sp)]
    sp_sources = [lax.rem(sp + n_sp - k, n_sp) for k in range(1, n_sp)]
    for t in [partner] + chip_peers:
        pl.semaphore_signal(barrier, inc=1, device_id=(sp, t), device_id_type=MESH)
    for s in sp_peers:
        pl.semaphore_signal(barrier, inc=1, device_id=(s, tp), device_id_type=MESH)
    pl.semaphore_wait(barrier, half + n_sp - 1)

    def remote(src, dst, send, recv, device):
        return pltpu.make_async_remote_copy(
            src_ref=src,
            dst_ref=dst,
            send_sem=send,
            recv_sem=recv,
            device_id=device,
            device_id_type=MESH,
        )

    sent = []

    def x_copy(layer, part, slot, sem, target):
        at, size = place(layer, part), chunk
        if layer == 0 and part == orders[0][0]:
            at, size = 0, chunk + GAIN_ROWS
        ref = xg[layer].at[slot, pl.ds(at, size)]
        return remote(ref, ref, sem, xr_sem.at[layer, part, slot], (sp, target))

    def begin(copy, condition=None):
        sent.append((copy, condition))
        if condition is None:
            copy.start()
        else:
            pl.when(condition)(copy.start)

    def x_start(layer, part):
        begin(x_copy(layer, part, tp, xf_sem.at[layer, part, tp], partner))
        for k in range(1, half):
            right = z + k <= half - (1 if k <= 2 else 2)
            left = z - k >= (0 if k <= 2 else 1)
            sem = xs_sem.at[layer, part, k]
            begin(x_copy(layer, part, tp, sem, tp + 2 * k), right)
            sem = xs_sem.at[layer, part, half + k]
            begin(x_copy(layer, part, tp, sem, tp - 2 * k), left)

    def x_finish(layer, part):
        for k in range(1, half):
            slot = lax.rem(tp + 2 * k, n_tp)
            relay = xl_sem.at[layer, part, slot]
            x_copy(layer, part, slot, relay, partner).wait_recv()
            right = x_copy(layer, part, slot, relay, tp + 2)
            begin(right, (slot < tp - 3) & (z == half - 2))
            left = x_copy(layer, part, slot, relay, tp - 2)
            begin(left, (slot > tp + 3) & (z == 1))
            begin(x_copy(layer, part, slot, xf_sem.at[layer, part, slot], partner))
        for k in range(half):
            slot = lax.rem(partner + 2 * k, n_tp)
            x_copy(layer, part, slot, xf_sem.at[layer, part, slot], partner).wait_recv()

    def w_copy(layer, which, slot, index, target):
        ref = (wkv, wqg)[which][layer].at[w_rows(slot)]
        return remote(
            ref, ref, ws_sem.at[layer, which, index], wr_sem.at[layer, which, slot], (target, tp)
        )

    def w_start(layer, which):
        for index, target in enumerate(sp_peers):
            begin(w_copy(layer, which, sp, index, target))

    def w_finish(layer, which):
        for slot in sp_sources:
            w_copy(layer, which, slot, 0, slot).wait_recv()

    def down(layer):
        buf = kvp[layer]
        return remote(
            buf.at[pl.ds(tokens, low)],
            buf.at[pl.ds(0, low)],
            hs_sem.at[layer, 0],
            hr_sem.at[layer, 0],
            (lax.rem(sp + 1, n_sp), tp),
        )

    def up(layer):
        buf = kvp[layer]
        return remote(
            buf.at[pl.ds(low, below)],
            buf.at[pl.ds(low + tokens, below)],
            hs_sem.at[layer, 1],
            hr_sem.at[layer, 1],
            (lax.rem(sp + n_sp - 1, n_sp), tp),
        )

    has_next = sp < n_sp - 1
    has_previous = sp > 0

    def norm(layer, part):
        buf = xg[layer]
        for c in range(group):
            at = pl.ds(place(layer, part) + c * GRID_W, GRID_W)
            to = pl.ds(part * chunk + c * GRID_W, GRID_W)
            total = jnp.zeros((GRID_W, feat), jnp.float32)
            for s in range(n_tp):
                wide = buf[s, at, :].astype(jnp.float32)
                total = total + wide * wide
            mean = jnp.sum(total, axis=-1, keepdims=True) * (1.0 / (n_tp * feat))
            scale = lax.rsqrt(mean + epsilon)
            for s in range(n_tp):
                gain = xg_a[s, 0:GAIN_ROWS, :][layer : layer + 1, :]
                wide = buf[s, at, :].astype(jnp.float32)
                normed[to, s * feat : (s + 1) * feat] = (
                    wide * scale * gain.astype(jnp.float32)
                ).astype(jnp.bfloat16)

    def project(weights, dst, offset, part):
        made = jnp.dot(
            normed[part * chunk : (part + 1) * chunk, :],
            weights[...],
            preferred_element_type=jnp.float32,
        )
        dst[pl.ds(offset + part * chunk, chunk), :] = made.astype(jnp.bfloat16)

    def attend(layer, index):
        row = sp * rows_dev + index
        first = jnp.minimum(jnp.maximum(row - HALO, 0), total_rows - WIN_R)
        local = first - sp * rows_dev + HALO
        base = first - row + WIN_R - 1
        at = pl.ds(pl.multiple_of(local * GRID_W, GRID_W), WIN_R * GRID_W)
        keys = kvp[layer][at, 0:feat]
        values = kvp[layer][at, feat : 2 * feat]
        query = q_buf[index * GRID_W : (index + 1) * GRID_W, :]
        scores = lax.dot_general(
            query, keys, (((1,), (1,)), ((), ())), preferred_element_type=jnp.float32
        )
        bias = jnp.concatenate([tiles[layer][base + 2 * j] for j in range(WIN_R // 2)], axis=1)
        scores = scores * factor + bias
        top = jnp.max(scores, axis=-1, keepdims=True)
        weight = jnp.exp(scores - top)
        weight = weight * (1.0 / jnp.sum(weight, axis=-1, keepdims=True))
        out = jnp.dot(weight.astype(jnp.bfloat16), values, preferred_element_type=jnp.float32)
        start = place(layer, index // group) + index % group * GRID_W
        wide = xg[layer][tp, pl.ds(start, GRID_W), :].astype(jnp.float32)
        return (wide + out).astype(jnp.bfloat16)

    for load, part in zip(loads, orders[0]):
        load.wait()
        x_start(0, part)
    rest = loads[count:]
    rest[0].wait()
    rest[1].wait()
    w_start(0, 0)
    rest[2].wait()
    w_start(0, 1)
    build_bias(table_a, rows_buf, tiles_a)
    build_bias(table_b, rows_buf, tiles_b)
    for load in rest[3:]:
        load.wait()

    top_rows = [i for i in range(rows_dev) if i < HALO]
    end_rows = [i for i in range(rows_dev) if i + HALO > rows_dev]
    up_parts = {i // group for i in range(below // GRID_W)}
    down_parts = {i // group for i in range(rows_dev - HALO, rows_dev)}

    for layer in range(2):
        done = set()
        for part in orders[layer]:
            x_finish(layer, part)
            norm(layer, part)
            if not done:
                w_finish(layer, 0)
            project(wkv[layer], kvp[layer], low, part)
            before = set(done)
            done.add(part)
            if down_parts <= done and not down_parts <= before:
                pl.when(has_next)(down(layer).start)
            if up_parts <= done and not up_parts <= before:
                pl.when(has_previous)(up(layer).start)
        if layer == 0:
            w_start(1, 0)
            w_start(1, 1)
        w_finish(layer, 1)
        for part in orders[layer]:
            project(wqg[layer], q_buf, 0, part)

        late = end_rows if layer == 0 else top_rows
        early = top_rows if layer == 0 else end_rows
        early = [i for i in early if i not in late]
        inner = [i for i in range(rows_dev) if i not in late and i not in early]
        finished = set()
        for rows, wait in ((inner, None), (early, layer == 0), (late, layer == 1)):
            if wait is True:
                pl.when(has_previous)(down(layer).wait_recv)
            if wait is False:
                pl.when(has_next)(up(layer).wait_recv)
            for index in rows:
                made = attend(layer, index)
                here = pl.ds(index * GRID_W, GRID_W)
                if layer == 1:
                    out_ref[here, :] = made
                    continue
                xg_b[tp, here, :] = made
                finished.add(index)
                part = index // group
                if all(part * group + i in finished for i in range(group)):
                    x_start(1, part)

    for layer in range(2):
        pl.when(has_next)(down(layer).wait_send)
        pl.when(has_previous)(up(layer).wait_send)
    for copy, condition in sent:
        if condition is None:
            copy.wait_send()
        else:
            pl.when(condition)(copy.wait_send)


def body(n_sp, n_tp, stream, gain_a, wq_a, wk_a, wv_a, table_a, gain_b, wq_b, wk_b, wv_b, table_b):
    tokens, feat = stream.shape
    depth = wq_a.shape[0] * n_sp
    rows_dev = tokens // GRID_W
    parts = 2 if rows_dev % 2 == 0 else rows_dev
    bf16 = jnp.bfloat16
    padded = tokens + 2 * HALO * GRID_W
    hbm = pl.BlockSpec(memory_space=pl.ANY)
    vmem = pl.BlockSpec(memory_space=pltpu.VMEM)
    dma = pltpu.SemaphoreType.DMA
    return pl.pallas_call(
        functools.partial(kernel, n_sp, n_tp),
        out_shape=pltpu.VMEM((tokens, feat), bf16),
        in_specs=[hbm] + [vmem] * 2 + [hbm] * 6 + [vmem] * 2,
        out_specs=vmem,
        scratch_shapes=[
            pltpu.VMEM((n_tp, tokens + GAIN_ROWS, feat), bf16),
            pltpu.VMEM((n_tp, tokens, feat), bf16),
            pltpu.VMEM((depth, 2 * feat), bf16),
            pltpu.VMEM((depth, 2 * feat), bf16),
            pltpu.VMEM((depth, feat), bf16),
            pltpu.VMEM((depth, feat), bf16),
            pltpu.VMEM((padded, 2 * feat), bf16),
            pltpu.VMEM((padded, 2 * feat), bf16),
            pltpu.VMEM((tokens, feat), bf16),
            pltpu.VMEM((tokens, n_tp * feat), bf16),
            pltpu.VMEM((2 * WIN_R, 2 * GRID_W), jnp.float32),
            pltpu.VMEM((2 * WIN_R - 2, GRID_W, 2 * GRID_W), jnp.float32),
            pltpu.VMEM((2 * WIN_R - 2, GRID_W, 2 * GRID_W), jnp.float32),
            dma((parts + 6,)),
            dma((2, parts, n_tp)),
            dma((2, parts, n_tp)),
            dma((2, parts, n_tp)),
            dma((2, parts, n_tp)),
            dma((2, 2, n_sp)),
            dma((2, 2, n_sp)),
            dma((2, 2)),
            dma((2, 2)),
        ],
        compiler_params=pltpu.CompilerParams(collective_id=0, has_side_effects=True),
    )(
        stream,
        gain_a.reshape(1, feat),
        gain_b.reshape(1, feat),
        wq_a,
        wk_a,
        wv_a,
        wq_b,
        wk_b,
        wv_b,
        jnp.transpose(table_a, (1, 0, 2)),
        jnp.transpose(table_b, (1, 0, 2)),
    )


def solution(mesh):
    placed = (
        P("sp", "tp"),
        P("tp"),
        P("sp", "tp"),
        P("sp", "tp"),
        P("sp", "tp"),
        P("tp", None, None),
        P("tp"),
        P("sp", "tp"),
        P("sp", "tp"),
        P("sp", "tp"),
        P("tp", None, None),
    )
    return jax.shard_map(
        functools.partial(body, mesh.shape["sp"], mesh.shape["tp"]),
        mesh=mesh,
        in_specs=placed,
        out_specs=P("sp", "tp"),
        check_vma=False,
    )
```

```python
import functools

import jax
import jax.numpy as jnp
from jax import lax
from jax.experimental import pallas as pl
from jax.experimental.pallas import tpu as pltpu
from jax.sharding import PartitionSpec as P

GRID_W = 64
WIN_R = 8
WIN_C = 16
HALO = 4
BATCH = 4
GAIN_ROWS = 16
epsilon = 1e-06
MESH = pl.DeviceIdType.MESH


def build_bias(table_ref, rows_ref, tiles_ref):
    rows_ref[...] = jnp.zeros_like(rows_ref)
    rows_ref[0 : 2 * WIN_R - 1, 0 : 2 * WIN_C - 1] = table_ref[:, 0, :]
    shape = (GRID_W, 2 * GRID_W)
    column = lax.broadcasted_iota(jnp.int32, shape, 0)
    key_column = lax.broadcasted_iota(jnp.int32, shape, 1)
    key_column = jnp.where(key_column >= GRID_W, key_column - GRID_W, key_column)
    start = jnp.clip(column - WIN_C // 2, 0, GRID_W - WIN_C)
    inside = (key_column >= start) & (key_column < start + WIN_C)
    for o in range(2 * WIN_R - 2):
        pair = rows_ref[o : o + 1, :] + pltpu.roll(rows_ref[o + 1 : o + 2, :], GRID_W, 1)
        tile = pltpu.roll(
            jnp.broadcast_to(pair, shape), 2 * GRID_W - (WIN_C - 1), 1, stride=1, stride_axis=0
        )
        tiles_ref[o] = jnp.where(inside, tile, -1e30)


def kernel(
    n_sp,
    n_tp,
    x_ref,
    gain_a,
    gain_b,
    wq_a,
    wk_a,
    wv_a,
    wq_b,
    wk_b,
    wv_b,
    table_a,
    table_b,
    out_ref,
    xg_a,
    xg_b,
    wkv_a,
    wkv_b,
    wqg_a,
    wqg_b,
    kvp_a,
    kvp_b,
    q_buf,
    normed,
    rows_buf,
    tiles_a,
    tiles_b,
    load_sem,
    xs_sem,
    xf_sem,
    xl_sem,
    xr_sem,
    ws_sem,
    wr_sem,
    hs_sem,
    hr_sem,
):
    sp = lax.axis_index("sp")
    tp = lax.axis_index("tp")
    tokens, feat = x_ref.shape
    depth = wq_a.shape[0]
    rows_dev = tokens // GRID_W
    total_rows = rows_dev * n_sp
    half = n_tp // 2
    core = lax.rem(tp, 2)
    z = tp // 2
    group = rows_dev // 2 if rows_dev % 2 == 0 else 1
    chunk = group * GRID_W
    count = rows_dev // group
    low_half = tuple(range(count // 2, count)) + tuple(range(count // 2))
    orders = (low_half, tuple(range(count)))
    partner = tp + 1 - 2 * core
    low = HALO * GRID_W
    below = (HALO - 1 if rows_dev >= WIN_R else HALO) * GRID_W
    factor = feat ** (-0.5)

    xg = (xg_a, xg_b)
    wkv = (wkv_a, wkv_b)
    wqg = (wqg_a, wqg_b)
    kvp = (kvp_a, kvp_b)
    tiles = (tiles_a, tiles_b)

    def w_rows(device):
        return pl.ds(pl.multiple_of(device * depth, depth), depth)

    mine = w_rows(sp)
    def place(layer, part):
        if layer == 1:
            return part * chunk
        return GAIN_ROWS + orders[0].index(part) * chunk

    loads = [
        (x_ref.at[pl.ds(part * chunk, chunk)], xg_a.at[tp, pl.ds(place(0, part), chunk)])
        for part in orders[0]
    ] + [
        (wk_a, wkv_a.at[mine, pl.ds(0, feat)]),
        (wv_a, wkv_a.at[mine, pl.ds(feat, feat)]),
        (wq_a, wqg_a.at[mine]),
        (wk_b, wkv_b.at[mine, pl.ds(0, feat)]),
        (wv_b, wkv_b.at[mine, pl.ds(feat, feat)]),
        (wq_b, wqg_b.at[mine]),
    ]
    loads = [pltpu.make_async_copy(s, d, load_sem.at[i]) for i, (s, d) in enumerate(loads)]
    for load in loads:
        load.start()
    spare = jnp.zeros((GAIN_ROWS - 2, feat), jnp.float32)
    both = [gain_a[...].astype(jnp.float32), gain_b[...].astype(jnp.float32), spare]
    xg_a[tp, 0:GAIN_ROWS, :] = jnp.concatenate(both, axis=0).astype(jnp.bfloat16)

    barrier = pltpu.get_barrier_semaphore()
    chip_peers = [lax.rem(tp + 2 * k, n_tp) for k in range(1, half)]
    sp_peers = [lax.rem(sp + k, n_sp) for k in range(1, n_sp)]
    sp_sources = [lax.rem(sp + n_sp - k, n_sp) for k in range(1, n_sp)]
    ends = int(half >= 4)
    at_end = (z == 0) | (z == half - 1)
    pl.semaphore_signal(barrier, inc=1, device_id=(sp, partner), device_id_type=MESH)

    def greet(target):
        pl.semaphore_signal(barrier, inc=1, device_id=(sp, target), device_id_type=MESH)

    for k, t in enumerate(chip_peers, 1):
        opposite = ((z == 0) & (k == half - 1)) | ((z == half - 1) & (k == 1))
        if ends:
            pl.when(jnp.logical_not(opposite))(functools.partial(greet, t))
        else:
            greet(t)
    for s in sp_peers:
        pl.semaphore_signal(barrier, inc=1, device_id=(s, tp), device_id_type=MESH)
    pl.semaphore_wait(barrier, half + n_sp - 1 - ends * at_end.astype(jnp.int32))

    def remote(src, dst, send, recv, device):
        return pltpu.make_async_remote_copy(
            src_ref=src,
            dst_ref=dst,
            send_sem=send,
            recv_sem=recv,
            device_id=device,
            device_id_type=MESH,
        )

    sent = []

    def x_copy(layer, part, slot, sem, target):
        at, size = place(layer, part), chunk
        if layer == 0 and part == orders[0][0]:
            at, size = 0, chunk + GAIN_ROWS
        ref = xg[layer].at[slot, pl.ds(at, size)]
        return remote(ref, ref, sem, xr_sem.at[layer, part, slot], (sp, target))

    def begin(copy, condition=None):
        sent.append((copy, condition))
        if condition is None:
            copy.start()
        else:
            pl.when(condition)(copy.start)

    def x_start(layer, part):
        begin(x_copy(layer, part, tp, xf_sem.at[layer, part, tp], partner))
        for k in range(1, half):
            right = z + k <= half - (1 if k <= 2 else 2)
            left = z - k >= (0 if k <= 2 else 1)
            sem = xs_sem.at[layer, part, k]
            begin(x_copy(layer, part, tp, sem, tp + 2 * k), right)
            sem = xs_sem.at[layer, part, half + k]
            begin(x_copy(layer, part, tp, sem, tp - 2 * k), left)

    def x_finish(layer, part):
        near = 1 - 2 * ((2 * z) // half)
        for k in range(1, half):
            slot = lax.rem(tp + n_tp + 2 * k * near, n_tp)
            relay = xl_sem.at[layer, part, slot]
            x_copy(layer, part, slot, relay, partner).wait_recv()
            right = x_copy(layer, part, slot, relay, tp + 2)
            begin(right, (slot < tp - 3) & (z == half - 2))
            left = x_copy(layer, part, slot, relay, tp - 2)
            begin(left, (slot > tp + 3) & (z == 1))
            begin(x_copy(layer, part, slot, xf_sem.at[layer, part, slot], partner))
        for k in range(half):
            slot = lax.rem(partner + n_tp + 2 * k * near, n_tp)
            x_copy(layer, part, slot, xf_sem.at[layer, part, slot], partner).wait_recv()

    def w_copy(layer, which, slot, index, target):
        ref = (wkv, wqg)[which][layer].at[w_rows(slot)]
        return remote(
            ref, ref, ws_sem.at[layer, which, index], wr_sem.at[layer, which, slot], (target, tp)
        )

    def w_start(layer, which):
        for index, target in enumerate(sp_peers):
            begin(w_copy(layer, which, sp, index, target))

    def w_finish(layer, which):
        for slot in sp_sources:
            w_copy(layer, which, slot, 0, slot).wait_recv()

    def down(layer):
        buf = kvp[layer]
        return remote(
            buf.at[pl.ds(tokens, low)],
            buf.at[pl.ds(0, low)],
            hs_sem.at[layer, 0],
            hr_sem.at[layer, 0],
            (lax.rem(sp + 1, n_sp), tp),
        )

    def up(layer):
        buf = kvp[layer]
        return remote(
            buf.at[pl.ds(low, below)],
            buf.at[pl.ds(low + tokens, below)],
            hs_sem.at[layer, 1],
            hr_sem.at[layer, 1],
            (lax.rem(sp + n_sp - 1, n_sp), tp),
        )

    has_next = sp < n_sp - 1
    has_previous = sp > 0

    def norm(layer, part):
        buf = xg[layer]
        for c in range(group):
            at = pl.ds(place(layer, part) + c * GRID_W, GRID_W)
            to = pl.ds(part * chunk + c * GRID_W, GRID_W)
            total = jnp.zeros((GRID_W, feat), jnp.float32)
            for s in range(n_tp):
                wide = buf[s, at, :].astype(jnp.float32)
                total = total + wide * wide
            mean = jnp.sum(total, axis=-1, keepdims=True) * (1.0 / (n_tp * feat))
            scale = lax.rsqrt(mean + epsilon)
            for s in range(n_tp):
                gain = xg_a[s, 0:GAIN_ROWS, :][layer : layer + 1, :]
                wide = buf[s, at, :].astype(jnp.float32)
                normed[to, s * feat : (s + 1) * feat] = (
                    wide * scale * gain.astype(jnp.float32)
                ).astype(jnp.bfloat16)

    def project(weights, dst, offset, part):
        made = jnp.dot(
            normed[part * chunk : (part + 1) * chunk, :],
            weights[...],
            preferred_element_type=jnp.float32,
        )
        dst[pl.ds(offset + part * chunk, chunk), :] = made.astype(jnp.bfloat16)

    def attend(layer, indices):
        places, scores = [], []
        for index in indices:
            row = sp * rows_dev + index
            first = jnp.minimum(jnp.maximum(row - HALO, 0), total_rows - WIN_R)
            local = first - sp * rows_dev + HALO
            base = first - row + WIN_R - 1
            at = pl.ds(pl.multiple_of(local * GRID_W, GRID_W), WIN_R * GRID_W)
            query = q_buf[index * GRID_W : (index + 1) * GRID_W, :]
            raw = lax.dot_general(
                query,
                kvp[layer][at, 0:feat],
                (((1,), (1,)), ((), ())),
                preferred_element_type=jnp.float32,
            )
            bias = jnp.concatenate([tiles[layer][base + 2 * j] for j in range(WIN_R // 2)], axis=1)
            places.append(at)
            scores.append(raw * factor + bias)
        tops = [jnp.max(score, axis=-1, keepdims=True) for score in scores]
        weights = [jnp.exp(score - top) for score, top in zip(scores, tops)]
        scales = [1.0 / jnp.sum(weight, axis=-1, keepdims=True) for weight in weights]
        outs = [
            jnp.dot(
                (weight * scale).astype(jnp.bfloat16),
                kvp[layer][at, feat : 2 * feat],
                preferred_element_type=jnp.float32,
            )
            for weight, scale, at in zip(weights, scales, places)
        ]
        made = []
        for index, out in zip(indices, outs):
            start = place(layer, index // group) + index % group * GRID_W
            wide = xg[layer][tp, pl.ds(start, GRID_W), :].astype(jnp.float32)
            made.append((wide + out).astype(jnp.bfloat16))
        return made

    for load, part in zip(loads, orders[0]):
        load.wait()
        x_start(0, part)
    rest = loads[count:]
    rest[0].wait()
    rest[1].wait()
    w_start(0, 0)
    rest[2].wait()
    w_start(0, 1)
    build_bias(table_a, rows_buf, tiles_a)
    build_bias(table_b, rows_buf, tiles_b)
    for load in rest[3:]:
        load.wait()

    top_rows = [i for i in range(rows_dev) if i < HALO]
    end_rows = [i for i in range(rows_dev) if i + HALO > rows_dev]
    up_parts = {i // group for i in range(below // GRID_W)}
    down_parts = {i // group for i in range(rows_dev - HALO, rows_dev)}

    for layer in range(2):
        done = set()
        for part in orders[layer]:
            x_finish(layer, part)
            norm(layer, part)
            if not done:
                w_finish(layer, 0)
            project(wkv[layer], kvp[layer], low, part)
            before = set(done)
            done.add(part)
            if down_parts <= done and not down_parts <= before:
                pl.when(has_next)(down(layer).start)
            if up_parts <= done and not up_parts <= before:
                pl.when(has_previous)(up(layer).start)
        if layer == 0:
            w_start(1, 0)
            w_start(1, 1)
        w_finish(layer, 1)
        for part in orders[layer]:
            project(wqg[layer], q_buf, 0, part)

        late = end_rows if layer == 0 else top_rows
        early = top_rows if layer == 0 else end_rows
        early = [i for i in early if i not in late]
        inner = [i for i in range(rows_dev) if i not in late and i not in early]
        finished = set()
        for rows, wait in ((inner, None), (early, layer == 0), (late, layer == 1)):
            if wait is True:
                pl.when(has_previous)(down(layer).wait_recv)
            if wait is False:
                pl.when(has_next)(up(layer).wait_recv)
            for index in rows:
                if (index - rows[0]) % BATCH == 0:
                    batch = [i for i in rows if index <= i < index + BATCH]
                    results = dict(zip(batch, attend(layer, batch)))
                here = pl.ds(index * GRID_W, GRID_W)
                if layer == 1:
                    out_ref[here, :] = results[index]
                    continue
                xg_b[tp, here, :] = results[index]
                finished.add(index)
                part = index // group
                if all(part * group + i in finished for i in range(group)):
                    x_start(1, part)

    for layer in range(2):
        pl.when(has_next)(down(layer).wait_send)
        pl.when(has_previous)(up(layer).wait_send)
    for copy, condition in sent:
        if condition is None:
            copy.wait_send()
        else:
            pl.when(condition)(copy.wait_send)


def body(n_sp, n_tp, stream, gain_a, wq_a, wk_a, wv_a, table_a, gain_b, wq_b, wk_b, wv_b, table_b):
    tokens, feat = stream.shape
    depth = wq_a.shape[0] * n_sp
    rows_dev = tokens // GRID_W
    parts = 2 if rows_dev % 2 == 0 else rows_dev
    bf16 = jnp.bfloat16
    padded = tokens + 2 * HALO * GRID_W
    hbm = pl.BlockSpec(memory_space=pl.ANY)
    vmem = pl.BlockSpec(memory_space=pltpu.VMEM)
    dma = pltpu.SemaphoreType.DMA
    return pl.pallas_call(
        functools.partial(kernel, n_sp, n_tp),
        out_shape=pltpu.VMEM((tokens, feat), bf16),
        in_specs=[hbm] + [vmem] * 2 + [hbm] * 6 + [vmem] * 2,
        out_specs=vmem,
        scratch_shapes=[
            pltpu.VMEM((n_tp, tokens + GAIN_ROWS, feat), bf16),
            pltpu.VMEM((n_tp, tokens, feat), bf16),
            pltpu.VMEM((depth, 2 * feat), bf16),
            pltpu.VMEM((depth, 2 * feat), bf16),
            pltpu.VMEM((depth, feat), bf16),
            pltpu.VMEM((depth, feat), bf16),
            pltpu.VMEM((padded, 2 * feat), bf16),
            pltpu.VMEM((padded, 2 * feat), bf16),
            pltpu.VMEM((tokens, feat), bf16),
            pltpu.VMEM((tokens, n_tp * feat), bf16),
            pltpu.VMEM((2 * WIN_R, 2 * GRID_W), jnp.float32),
            pltpu.VMEM((2 * WIN_R - 2, GRID_W, 2 * GRID_W), jnp.float32),
            pltpu.VMEM((2 * WIN_R - 2, GRID_W, 2 * GRID_W), jnp.float32),
            dma((parts + 6,)),
            dma((2, parts, n_tp)),
            dma((2, parts, n_tp)),
            dma((2, parts, n_tp)),
            dma((2, parts, n_tp)),
            dma((2, 2, n_sp)),
            dma((2, 2, n_sp)),
            dma((2, 2)),
            dma((2, 2)),
        ],
        compiler_params=pltpu.CompilerParams(collective_id=0, has_side_effects=True),
    )(
        stream,
        gain_a.reshape(1, feat),
        gain_b.reshape(1, feat),
        wq_a,
        wk_a,
        wv_a,
        wq_b,
        wk_b,
        wv_b,
        jnp.transpose(table_a, (1, 0, 2)),
        jnp.transpose(table_b, (1, 0, 2)),
    )


def solution(mesh):
    placed = (
        P("sp", "tp"),
        P("tp"),
        P("sp", "tp"),
        P("sp", "tp"),
        P("sp", "tp"),
        P("tp", None, None),
        P("tp"),
        P("sp", "tp"),
        P("sp", "tp"),
        P("sp", "tp"),
        P("tp", None, None),
    )
    return jax.shard_map(
        functools.partial(body, mesh.shape["sp"], mesh.shape["tp"]),
        mesh=mesh,
        in_specs=placed,
        out_specs=P("sp", "tp"),
        check_vma=False,
    )
```
